32 devices in a mesh: grp: 2 (over y), sp: 8 (over z, x), tp: 2 (over core).
Axes of the slice: x: 2, y: 2, z: 4, core: 2. Of those that a mesh axis runs over, the one named last changes fastest.
Arguments:
- layer_input: bfloat16 [4, 1024, 2048], P('grp', ('sp', 'tp')), parts along dimension 0, may hold values from -6 to 6
- norm_gain: float32 [2048], replicated, may hold values from 0.1 to 1.9
- in_weight: bfloat16 [2048, 1024], P(None, 'tp'), may hold values from -0.125 to 0.125
- gate_weight: bfloat16 [2048, 1024], P(None, 'tp'), may hold values from -0.125 to 0.125
- rate_real: float32 [64, 64], P('tp'), may hold values from -1 to 0
- rate_imag: float32 [64, 64], P('tp'), may hold values from -3 to 3
- log_step: float32 [64], P('tp'), may hold values from -8 to -2.5
- input_real: bfloat16 [64, 64, 16], P('tp'), may hold values from -4 to 4
- input_imag: bfloat16 [64, 64, 16], P('tp'), may hold values from -4 to 4
- output_real: bfloat16 [64, 16, 64], P('tp'), may hold values from -10 to 10
- output_imag: bfloat16 [64, 16, 64], P('tp'), may hold values from -10 to 10
- skip_weight: float32 [1024], P('tp'), may hold values from -20 to 20
- decay_offset: float32 [4, 1024, 64], P('grp', 'sp', 'tp'), parts along dimension 0, may hold values from -1.5 to 0
- channel_gain: float32 [1024], replicated, may hold values from 0.1 to 1.9
- out_weight: bfloat16 [1024, 2048], P('tp'), may hold values from -0.1875 to 0.1875
Outputs:
- layer_output: bfloat16 [4, 1024, 2048], P('grp', ('sp', 'tp')), parts along dimension 0
The draws below stay inside these ranges and needn't reach their ends.
There are 2 independent parts, one for each index of `grp`. The reference program is written for one: setup_inputs(seed, part) draws one part's arguments, and reference() takes and returns one part's arrays. A program takes and returns all parts, laid end to end along the dimension named above; an argument that names none is the same for every part. Nothing has to cross between parts.
All inputs are finite; a program needn't handle non-finite values.
Results may differ from the reference program's by a relative error of at most 0.014.
Values may be sent and summed in bfloat16 or wider, within the bound.
A program may use at most 128 MiB of HBM per device.

```python
import math
import jax
import jax.numpy as jnp
from jax import lax

D = 2048
CHANNEL_GROUPS = 64
GROUP_CH = 16
STATE = 64
WIDTH = 1024
SEQUENCE_COUNT = 2
POS_DEV = 128
SEQUENCE_LENGTH = 1024


def group_speed(key):
    ranking = jax.random.permutation(jax.random.fold_in(key, 101), CHANNEL_GROUPS)
    fast_count = CHANNEL_GROUPS // 2
    return (ranking >= fast_count).astype(jnp.float32)


def group_scales():
    exponent = lax.iota(jnp.float32, CHANNEL_GROUPS) / (CHANNEL_GROUPS - 1)
    spread_base = 3.0
    return spread_base ** exponent


def draw_rate_real(key, part):
    slow_mask = group_speed(key)[:, None]
    slow_rate = -jnp.exp(jax.random.uniform(jax.random.fold_in(key, 3), (CHANNEL_GROUPS, STATE), jnp.float32, math.log(0.5), 0.0)) * math.sqrt(5.0 / SEQUENCE_LENGTH)
    fast_rate = -jax.random.uniform(jax.random.fold_in(key, 4), (CHANNEL_GROUPS, STATE), jnp.float32, 0.25, 1.0)
    return slow_mask * slow_rate + (1.0 - slow_mask) * fast_rate


def draw_log_step(key, part):
    slow_mask = group_speed(key)
    jitter = jax.random.uniform(jax.random.fold_in(key, 5), (CHANNEL_GROUPS,), jnp.float32, -0.2, 0.2)
    slow_value = math.log(0.07 * math.sqrt(5.0 / SEQUENCE_LENGTH))
    fast_value = math.log(0.05)
    return slow_mask * slow_value + (1.0 - slow_mask) * fast_value + jitter


def output_table(key, salt):
    values = jax.random.truncated_normal(jax.random.fold_in(key, salt), -4.0, 4.0, (CHANNEL_GROUPS, GROUP_CH, STATE), jnp.float32)
    return values * 0.25 * group_scales()[:, None, None]


def draw_output_real(key, part):
    return output_table(key, 31).astype(jnp.bfloat16)


def draw_output_imag(key, part):
    return output_table(key, 32).astype(jnp.bfloat16)


def draw_skip_weight(key, part):
    values = jax.random.truncated_normal(jax.random.fold_in(key, 41), -4.0, 4.0, (WIDTH,), jnp.float32)
    return values * 0.5 * jnp.repeat(group_scales(), GROUP_CH)


def draw_decay_offset(key, part):
    block_count = SEQUENCE_LENGTH // POS_DEV
    block_scale = jnp.exp(jax.random.uniform(jax.random.fold_in(key, 21), (SEQUENCE_COUNT, block_count, CHANNEL_GROUPS), jnp.float32, math.log(0.5), math.log(4.0)))
    block_scale = jnp.repeat(block_scale, POS_DEV, axis=1)
    roughness = jax.random.uniform(jax.random.fold_in(key, 22), (SEQUENCE_COUNT, SEQUENCE_LENGTH, CHANNEL_GROUPS), jnp.float32, 0.5, 1.5)
    steady = -(0.2 / SEQUENCE_LENGTH) * block_scale * roughness
    spike_location = jax.random.randint(jax.random.fold_in(key, 23), (SEQUENCE_COUNT, 2, CHANNEL_GROUPS), 0, SEQUENCE_LENGTH)
    spike_depth = jax.random.uniform(jax.random.fold_in(key, 24), (SEQUENCE_COUNT, 2, CHANNEL_GROUPS), jnp.float32, 0.22, 0.69)
    token_position = lax.iota(jnp.int32, SEQUENCE_LENGTH)[None, :, None]
    loss_values = jnp.where(token_position == spike_location[:, 0:1, :], spike_depth[:, 0:1, :], 0.0) + jnp.where(token_position == spike_location[:, 1:2, :], spike_depth[:, 1:2, :], 0.0)
    return steady - loss_values


def shard_levels(rng, dims, shards, least, largest):
    def one(axis_at, blocks):
        steps = jax.random.uniform(jax.random.fold_in(jax.random.fold_in(rng, 6), axis_at), (blocks,), jnp.float32, least / len(shards), largest / len(shards))
        return jnp.repeat(jnp.exp(steps), dims[axis_at] // blocks).reshape((-1,) + (1,) * (len(dims) - axis_at - 1))

    loudness = one(*shards[0])
    for cut in shards[1:]:
        loudness = loudness * one(*cut)
    return loudness


def gaussian(stream_key, dims, deviation, reach, shards=(), kind=jnp.bfloat16):
    result = deviation * jax.random.normal(stream_key, dims, jnp.float32)
    if shards:
        result = result * shard_levels(stream_key, dims, shards, -0.22, 0.18)
    return jnp.clip(result, -reach, reach).astype(kind)


def setup_inputs(seed: int = 0, part: int = 0) -> dict:
    seeds = jax.random.split(jax.random.key(seed), 16)
    own_keys = jax.random.split(jax.random.fold_in(seeds[15], part), 16)
    layer_input = gaussian(own_keys[0], (SEQUENCE_COUNT, SEQUENCE_LENGTH, D), 1.0, 6.0, ((1, 16),))
    norm_gain = jnp.clip(1.0 + 0.18 * jax.random.normal(seeds[1], (D,), jnp.float32), 0.1, 1.9)
    in_weight = gaussian(seeds[2], (D, WIDTH), D ** -0.5, 0.125, ((1, 2),))
    gate_weight = gaussian(seeds[3], (D, WIDTH), D ** -0.5, 0.125, ((1, 2),))
    rate_real = draw_rate_real(jax.random.fold_in(seeds[15], 71), part)
    rate_imag = jnp.clip(jax.random.uniform(seeds[5], (CHANNEL_GROUPS, STATE), jnp.float32, -3.0, 3.0) * shard_levels(seeds[5], (CHANNEL_GROUPS, STATE), ((0, 2),), -0.4, 0.0), -3.0, 3.0)
    log_step = draw_log_step(jax.random.fold_in(seeds[15], 71), part)
    input_real = gaussian(seeds[7], (CHANNEL_GROUPS, STATE, GROUP_CH), 0.25, 4.0, ((0, 2),))
    input_imag = gaussian(seeds[8], (CHANNEL_GROUPS, STATE, GROUP_CH), 0.25, 4.0, ((0, 2),))
    output_real = draw_output_real(jax.random.fold_in(seeds[15], 71), part)
    output_imag = draw_output_imag(jax.random.fold_in(seeds[15], 71), part)
    skip_weight = draw_skip_weight(jax.random.fold_in(seeds[15], 71), part)
    decay_offset = draw_decay_offset(jax.random.fold_in(jax.random.fold_in(seeds[15], part), 71), part)
    channel_gain = jnp.clip(1.0 + 0.18 * jax.random.normal(seeds[13], (WIDTH,), jnp.float32), 0.1, 1.9)
    out_weight = gaussian(seeds[14], (WIDTH, D), WIDTH ** -0.5, 0.1875, ((0, 2),))
    return dict(layer_input=layer_input, norm_gain=norm_gain, in_weight=in_weight, gate_weight=gate_weight, rate_real=rate_real, rate_imag=rate_imag, log_step=log_step, input_real=input_real, input_imag=input_imag, output_real=output_real, output_imag=output_imag, skip_weight=skip_weight, decay_offset=decay_offset, channel_gain=channel_gain, out_weight=out_weight)


epsilon = 1e-06
HIGHEST = lax.Precision.HIGHEST

def coefficients(rate_real, rate_imag, log_step, input_real, input_imag):
    step_size = jnp.exp(log_step)[:, None]
    real_step = rate_real * step_size
    angle_step = rate_imag * step_size
    top_re = jnp.expm1(real_step) * jnp.cos(angle_step) - 2.0 * jnp.sin(0.5 * angle_step) ** 2
    top_im = jnp.exp(real_step) * jnp.sin(angle_step)
    inverse = 1.0 / (rate_real * rate_real + rate_imag * rate_imag)
    coef_re = (top_re * rate_real + top_im * rate_imag) * inverse
    coef_im = (top_im * rate_real - top_re * rate_imag) * inverse
    table_re = input_real.astype(jnp.float32)
    table_im = input_imag.astype(jnp.float32)
    bbar_re = coef_re[..., None] * table_re - coef_im[..., None] * table_im
    bbar_im = coef_re[..., None] * table_im + coef_im[..., None] * table_re
    return (real_step, angle_step, bbar_re, bbar_im)

def compose(earlier, later):
    new_a_re = later[0] * earlier[0] - later[1] * earlier[1]
    new_a_im = later[0] * earlier[1] + later[1] * earlier[0]
    new_b_re = later[0] * earlier[2] - later[1] * earlier[3] + later[2]
    new_b_im = later[0] * earlier[3] + later[1] * earlier[2] + later[3]
    return (new_a_re, new_a_im, new_b_re, new_b_im)

def one_group(group_items):
    inputs_group, offset_group, real_row, rot_re, rot_im, bbar_re, bbar_im, read_re, read_im, skip_row = group_items
    magnitude = jnp.exp(real_row[None, None, :] + offset_group[..., None])
    trans_re = magnitude * rot_re[None, None, :]
    trans_im = magnitude * rot_im[None, None, :]
    drive_re = jnp.einsum('slc,pc->slp', inputs_group, bbar_re, precision=HIGHEST)
    drive_im = jnp.einsum('slc,pc->slp', inputs_group, bbar_im, precision=HIGHEST)
    scanned = lax.associative_scan(compose, (trans_re, trans_im, drive_re, drive_im), axis=1)
    mixed = jnp.einsum('slp,cp->slc', scanned[2], read_re, precision=HIGHEST) - jnp.einsum('slp,cp->slc', scanned[3], read_im, precision=HIGHEST)
    return mixed + skip_row[None, None, :] * inputs_group

def reference(layer_input, norm_gain, in_weight, gate_weight, rate_real, rate_imag, log_step, input_real, input_imag, output_real, output_imag, skip_weight, decay_offset, channel_gain, out_weight):
    wide_tokens = layer_input.astype(jnp.float32)
    normed = (wide_tokens * lax.rsqrt(lax.optimization_barrier(jnp.mean(wide_tokens * wide_tokens, axis=-1, keepdims=True)) + epsilon) * norm_gain).astype(jnp.bfloat16)
    flat_rows = normed.reshape(SEQUENCE_COUNT * SEQUENCE_LENGTH, D)
    inputs = jnp.dot(flat_rows, in_weight, preferred_element_type=jnp.float32).astype(jnp.bfloat16)
    gates = jnp.dot(flat_rows, gate_weight, preferred_element_type=jnp.float32).astype(jnp.bfloat16)
    inputs = inputs.reshape(SEQUENCE_COUNT, SEQUENCE_LENGTH, WIDTH)
    gates = gates.reshape(SEQUENCE_COUNT, SEQUENCE_LENGTH, WIDTH)
    real_step, angle_step, bbar_re, bbar_im = coefficients(rate_real, rate_imag, log_step, input_real, input_imag)
    inputs_wide = inputs.astype(jnp.float32)
    inputs_groups = jnp.moveaxis(inputs_wide.reshape(SEQUENCE_COUNT, SEQUENCE_LENGTH, CHANNEL_GROUPS, GROUP_CH), 2, 0)
    offset_groups = jnp.moveaxis(decay_offset, 2, 0)
    skip_groups = skip_weight.reshape(CHANNEL_GROUPS, GROUP_CH)
    mixed = lax.map(one_group, (inputs_groups, offset_groups, real_step, jnp.cos(angle_step), jnp.sin(angle_step), bbar_re, bbar_im, output_real.astype(jnp.float32), output_imag.astype(jnp.float32), skip_groups))
    mixed = jnp.moveaxis(mixed, 0, 2).reshape(SEQUENCE_COUNT, SEQUENCE_LENGTH, WIDTH)
    activated = jax.nn.gelu(mixed, approximate=False) * jax.nn.sigmoid(gates.astype(jnp.float32))
    normalized = (activated * lax.rsqrt(lax.optimization_barrier(jnp.mean(activated * activated, axis=-1, keepdims=True)) + epsilon) * channel_gain).astype(jnp.bfloat16)
    output = jnp.dot(normalized.reshape(SEQUENCE_COUNT * SEQUENCE_LENGTH, WIDTH), out_weight, preferred_element_type=jnp.float32)
    return output.astype(jnp.bfloat16).reshape(SEQUENCE_COUNT, SEQUENCE_LENGTH, D)
```

```python
import functools

import jax
import jax.numpy as jnp
from jax import lax
from jax.experimental import pallas as pl
from jax.experimental.pallas import tpu as pltpu
from jax.sharding import PartitionSpec as P

epsilon = 1e-06
HIGHEST = lax.Precision.HIGHEST
MESH = pl.DeviceIdType.MESH
F32 = jnp.float32
BF16 = jnp.bfloat16


def iota(shape, dim):
    return lax.broadcasted_iota(jnp.int32, shape, dim)


def cmul(a, b):
    return (a[0] * b[0] - a[1] * b[1], a[0] * b[1] + a[1] * b[0])


def cpow(a, k):
    result = None
    while k:
        if k & 1:
            result = a if result is None else cmul(result, a)
        k >>= 1
        if k:
            a = cmul(a, a)
    return result


def dot(a, b, precision=None):
    return jnp.dot(a, b, preferred_element_type=F32, precision=precision)


def dot_nt(a, b):
    return lax.dot_general(a, b, (((1,), (1,)), ((), ())), preferred_element_type=F32)


def kernel(
    sizes,
    x_hbm, ng, inw_hbm, gw_hbm, rr, ri, ls, bre, bim, cre, cim, skip, dec, cg, outw_hbm,
    out,
    xf, w_in, w_g, w_o, nrm, u_ref, gate_ref, rel_ref,
    bd_re, bd_im, cd_re, cd_im, ti_re, ti_im, to_re, to_im,
    p_re, p_im, xc_re, xc_im, tot, tot_all, st, st_all, act, act_in,
    load_sem, tp_send, tp_recv, tot_send, tot_recv, st_send, st_recv,
):
    n, tp, S, Q, D, G, N, C, tile_g, out_cols = sizes
    W = G * C
    tiles = G // tile_g
    cw, mw = tile_g * C, tile_g * N
    SQ = S * Q
    mid = Q // 2 - 1
    sp_me = lax.axis_index("sp")
    me = lax.axis_index("tp")
    peer = 1 - me

    barrier = pltpu.get_barrier_semaphore()
    pl.semaphore_signal(barrier, inc=1, device_id={"tp": peer}, device_id_type=MESH)

    def greet(i, carry):
        other = lax.rem(sp_me + 1 + i, n)
        pl.semaphore_signal(barrier, inc=1, device_id={"sp": other}, device_id_type=MESH)
        return carry

    lax.fori_loop(0, n - 1, greet, 0)

    load_x = pltpu.make_async_copy(x_hbm, xf.at[me], load_sem.at[0])
    load_in = pltpu.make_async_copy(inw_hbm, w_in, load_sem.at[1])
    load_g = pltpu.make_async_copy(gw_hbm, w_g, load_sem.at[2])
    load_o = pltpu.make_async_copy(outw_hbm, w_o.at[me], load_sem.at[3])
    load_x.start()
    load_in.start()
    load_g.start()
    load_o.start()

    tri = (iota((Q, Q), 0) >= iota((Q, Q), 1)).astype(F32)
    to_chan = (iota((G, W), 1) // C == iota((G, W), 0)).astype(F32)
    mids, lasts, totals = [], [], []
    tot[...] = jnp.zeros_like(tot)
    for s in range(S):
        total = None
        for c in range(tp):
            cum = dot(tri, dec[s, c * Q:(c + 1) * Q, :], HIGHEST)
            at_mid = cum[mid:mid + 1, :]
            at_end = cum[Q - 1:Q, :]
            mids.append(at_mid)
            lasts.append(at_end - at_mid)
            total = at_end if total is None else total + at_end
            rows = (c * S + s) * Q
            rel_ref[rows:rows + Q, :] = dot(cum - at_mid, to_chan, HIGHEST)
        totals.append(total)
        tot[s:s + 1, :] = total

    pl.semaphore_wait(barrier, n)

    load_x.wait()
    load_o.wait()
    send_x = pltpu.make_async_remote_copy(
        xf.at[me], xf.at[me], tp_send.at[0], tp_recv.at[0], device_id={"tp": peer}, device_id_type=MESH
    )
    send_o = pltpu.make_async_remote_copy(
        w_o.at[me], w_o.at[me], tp_send.at[1], tp_recv.at[1], device_id={"tp": peer}, device_id_type=MESH
    )
    send_x.start()
    send_o.start()

    def tot_copy(target):
        return pltpu.make_async_remote_copy(
            tot, tot_all.at[sp_me], tot_send.at[target], tot_recv.at[sp_me],
            device_id={"sp": target}, device_id_type=MESH,
        )

    def st_copy(target):
        return pltpu.make_async_remote_copy(
            st, st_all.at[sp_me], st_send.at[target], st_recv.at[sp_me],
            device_id={"sp": target}, device_id_type=MESH,
        )

    def to_later(act_on):
        def body(i, carry):
            act_on(n - 1 - i)
            return carry

        lax.fori_loop(0, n - 1 - sp_me, body, 0)

    to_later(lambda target: tot_copy(target).start())

    ls_row = jnp.broadcast_to(ls[...], (G, G))
    step = jnp.exp(jnp.sum(jnp.where(iota((G, G), 0) == iota((G, G), 1), ls_row, 0.0), axis=1, keepdims=True))
    rate_re, rate_im = rr[...], ri[...]
    real_step = rate_re * step
    angle_step = rate_im * step
    cosa, sina = jnp.cos(angle_step), jnp.sin(angle_step)
    half = jnp.sin(0.5 * angle_step)
    grown = jnp.exp(real_step)
    shrunk = jnp.exp(-real_step)
    series = jnp.ones_like(real_step)
    for k in range(11, 1, -1):
        series = 1.0 + real_step * (1.0 / k) * series
    minus_one = jnp.where(jnp.abs(real_step) < 0.5, real_step * series, grown - 1.0)
    top_re = minus_one * cosa - 2.0 * half * half
    top_im = grown * sina
    inverse = 1.0 / (rate_re * rate_re + rate_im * rate_im)
    coef_re = (top_re * rate_re + top_im * rate_im) * inverse
    coef_im = (top_im * rate_re - top_re * rate_im) * inverse
    spread = (iota((N, mw), 1) % N == iota((N, mw), 0)).astype(F32)
    to_mode = (iota((tile_g, mw), 1) // N == iota((tile_g, mw), 0)).astype(F32)

    def rows_of(item, q):
        wide = dot(item[q * tile_g:(q + 1) * tile_g, :], spread, HIGHEST)
        return jnp.sum(wide * to_mode, axis=0, keepdims=True)

    up_half, up_end, up_all = [], [], []
    k8 = iota((8, mw), 0)
    bmask = iota((mw, cw), 0) // N == iota((mw, cw), 1) // C
    cmask = iota((cw, mw), 0) // C == iota((cw, mw), 1) // N
    btile = (iota((C, cw), 1) % C == iota((C, cw), 0)).astype(BF16)
    ctile = spread.astype(BF16)

    def table(a, base, t_re, t_im, q):
        a2 = cmul(a, a)
        a4 = cmul(a2, a2)
        a8 = cmul(a4, a4)
        block = tuple(jnp.broadcast_to(b, (8, mw)) for b in base)
        for bit, power in ((1, a), (2, a2), (4, a4)):
            on = (k8 & bit) != 0
            block = cmul(block, (jnp.where(on, power[0], 1.0), jnp.where(on, power[1], 0.0)))
        for j in range(Q // 8):
            t_re[q, j * 8:j * 8 + 8, :] = block[0]
            t_im[q, j * 8:j * 8 + 8, :] = block[1]
            block = cmul(block, a8)

    for q in range(tiles):
        a = (rows_of(grown * cosa, q), rows_of(grown * sina, q))
        inv = (rows_of(shrunk * cosa, q), rows_of(-shrunk * sina, q))
        coef = (rows_of(coef_re, q), rows_of(coef_im, q))
        table(inv, cmul(coef, cpow(a, mid)), ti_re, ti_im, q)
        table(a, cpow(inv, mid), to_re, to_im, q)
        up_half.append(cpow(a, mid + 1))
        up_end.append(cpow(a, Q - 1 - mid))
        up_all.append(cpow(a, Q * tp))
        for src, dst in ((bre, bd_re), (bim, bd_im)):
            dst[q] = jnp.where(bmask, dot(src[q * mw:(q + 1) * mw, :], btile), 0.0).astype(BF16)
        for src, dst in ((cre, cd_re), (cim, cd_im)):
            dst[q] = jnp.where(cmask, dot(src[q * cw:(q + 1) * cw, :], ctile), 0.0).astype(BF16)

    row_tile = min(32, Q)

    def project(slot):
        first = slot * SQ

        def normalize(i, carry):
            s = i // (Q // row_tile)
            r = pl.multiple_of((i % (Q // row_tile)) * row_tile, row_tile)
            x = xf[slot, s, pl.ds(r, row_tile), :].astype(F32)
            scale = lax.rsqrt(jnp.mean(x * x, axis=-1, keepdims=True) + epsilon)
            rows = pl.ds(pl.multiple_of(first + i * row_tile, row_tile), row_tile)
            nrm[rows, :] = (x * scale * ng[...]).astype(BF16)
            return carry

        lax.fori_loop(0, SQ // row_tile, normalize, 0)
        rows = pl.ds(pl.multiple_of(first, SQ), SQ)
        u_ref[rows, :] = dot(nrm[rows, :], w_in[...]).astype(BF16)

    load_in.wait()
    project(me)
    send_x.wait_recv()
    project(peer)

    R = tp * SQ
    ri_, ci_ = iota((R, R), 0), iota((R, R), 1)
    chunk_tri = ((ri_ >= ci_) & (ri_ // Q == ci_ // Q)).astype(BF16)

    for q in range(tiles):
        cols = slice(q * cw, (q + 1) * cw)
        uq = (u_ref[:, cols].astype(F32) * jnp.exp(-rel_ref[:, cols])).astype(BF16)
        d_re = dot_nt(uq, bd_re[q]).reshape(tp * S, Q, mw)
        d_im = dot_nt(uq, bd_im[q]).reshape(tp * S, Q, mw)
        t = (ti_re[q][None], ti_im[q][None])
        z_re, z_im = cmul(t, (d_re, d_im))
        p_re[q] = dot(chunk_tri, z_re.reshape(R, mw).astype(BF16))
        p_im[q] = dot(chunk_tri, z_im.reshape(R, mw).astype(BF16))

    def widen(row, q):
        return jnp.exp(dot(jnp.broadcast_to(row[:, q * tile_g:(q + 1) * tile_g], (8, tile_g)), to_mode, HIGHEST)[0:1])

    enter_f, leave_f = {}, {}
    for q in range(tiles):
        for s in range(S):
            x = None
            for c in range(tp):
                b = c * S + s
                e_mid = widen(mids[s * tp + c], q)
                e_end = widen(lasts[s * tp + c], q)
                enter_f[q, s, c] = (up_half[q][0] * e_mid, up_half[q][1] * e_mid)
                leave_f[q, s, c] = (up_end[q][0] * e_end, up_end[q][1] * e_end)
                last = b * Q + Q - 1
                end = (p_re[q, last:last + 1, :], p_im[q, last:last + 1, :])
                if x is not None:
                    add = cmul(enter_f[q, s, c], x)
                    end = (end[0] + add[0], end[1] + add[1])
                x = cmul(leave_f[q, s, c], end)
            st[q, s:s + 1, :] = x[0].astype(BF16)
            st[q, S + s:S + s + 1, :] = x[1].astype(BF16)

    to_later(lambda target: st_copy(target).start())

    load_g.wait()
    gate_ref[...] = dot(nrm[...], w_g[...]).astype(BF16)

    def enter(j, x):
        pltpu.make_async_remote_copy(
            tot, tot_all.at[j], tot_send.at[j], tot_recv.at[j], device_id={"tp": peer}, device_id_type=MESH
        ).wait_recv()
        pltpu.make_async_remote_copy(
            st, st_all.at[j], st_send.at[j], st_recv.at[j], device_id={"tp": peer}, device_id_type=MESH
        ).wait_recv()
        logs = tot_all[j]
        new = []
        for q in range(tiles):
            decay = jnp.exp(dot(logs[:, q * tile_g:(q + 1) * tile_g], to_mode, HIGHEST))[0:S]
            got = st_all[j, q].astype(F32)
            re, im = cmul((up_all[q][0] * decay, up_all[q][1] * decay), x[q])
            new.append((re + got[0:S], im + got[S:2 * S]))
        return tuple(new)

    zero = jnp.zeros((S, mw), F32)
    entering = lax.fori_loop(0, sp_me, enter, tuple((zero, zero) for _ in range(tiles)))

    for q in range(tiles):
        for s in range(S):
            x = (entering[q][0][s:s + 1], entering[q][1][s:s + 1])
            for c in range(tp):
                b = c * S + s
                add = cmul(enter_f[q, s, c], x)
                xc_re[q, b:b + 1, :] = add[0]
                xc_im[q, b:b + 1, :] = add[1]
                if c < tp - 1:
                    last = b * Q + Q - 1
                    x = cmul(
                        leave_f[q, s, c],
                        (p_re[q, last:last + 1, :] + add[0], p_im[q, last:last + 1, :] + add[1]),
                    )

    def read_out(slot, dst):
        first = pl.multiple_of(slot * SQ, SQ)
        rows = pl.ds(first, SQ)
        for q in range(tiles):
            cols = slice(q * cw, (q + 1) * cw)
            acc_re, acc_im = [], []
            for s in range(S):
                block = pl.ds(pl.multiple_of(first + s * Q, Q), Q)
                one = pl.ds(slot * S + s, 1)
                v = (p_re[q, block, :] + xc_re[q, one, :], p_im[q, block, :] + xc_im[q, one, :])
                w = cmul((to_re[q], to_im[q]), v)
                acc_re.append(w[0].astype(BF16))
                acc_im.append(w[1].astype(BF16))
            w_re = jnp.concatenate(acc_re, axis=0)
            w_im = jnp.concatenate(acc_im, axis=0)
            y = dot_nt(w_re, cd_re[q]) - dot_nt(w_im, cd_im[q])
            mixed = y * jnp.exp(rel_ref[rows, cols]) + skip[:, cols] * u_ref[rows, cols].astype(F32)
            gate = jax.nn.sigmoid(gate_ref[rows, cols].astype(F32))
            gelu = 0.5 * mixed * (1.0 + lax.erf(mixed * 0.7071067811865476))
            dst[:, cols] = (gelu * gate).astype(BF16)

    read_out(peer, act.at[peer])
    send_a = pltpu.make_async_remote_copy(
        act.at[peer], act_in, tp_send.at[2], tp_recv.at[2], device_id={"tp": peer}, device_id_type=MESH
    )
    send_a.start()
    read_out(me, act.at[me])
    own = act[me].astype(F32)
    own_sq = jnp.sum(own * own, axis=-1, keepdims=True)
    own_g = (own * cg[me]).astype(BF16)
    send_o.wait_recv()
    send_a.wait_recv()
    got = act_in[...].astype(F32)
    got_sq = jnp.sum(got * got, axis=-1, keepdims=True)
    got_g = (got * cg[peer]).astype(BF16)
    scale = lax.rsqrt((own_sq + got_sq) * (1.0 / (tp * W)) + epsilon)
    for k in range(D // out_cols):
        cols = slice(k * out_cols, (k + 1) * out_cols)
        y = dot(own_g, w_o[me, :, cols]) + dot(got_g, w_o[peer, :, cols])
        out[:, :, cols] = (y * scale).astype(BF16).reshape(S, Q, out_cols)

    send_x.wait_send()
    send_o.wait_send()
    send_a.wait_send()
    to_later(lambda target: tot_copy(target).wait_send())
    to_later(lambda target: st_copy(target).wait_send())


def shards(
    n, tp, layer_input, norm_gain, in_weight, gate_weight, rate_real, rate_imag, log_step, input_real,
    input_imag, output_real, output_imag, skip_weight, decay_offset, channel_gain, out_weight,
):
    S, Q, D = layer_input.shape
    G, N = rate_real.shape
    C = input_real.shape[2]
    W = G * C
    tile_g = min(G, max(1, 128 // C))
    tiles = G // tile_g
    cw, mw = tile_g * C, tile_g * N
    R = tp * S * Q
    assert tp == 2 and Q <= 64 and Q % 8 == 0
    sizes = (n, tp, S, Q, D, G, N, C, tile_g, min(512, D))
    vmem = pl.BlockSpec(memory_space=pltpu.VMEM)
    hbm = pl.BlockSpec(memory_space=pl.ANY)
    dma = pltpu.SemaphoreType.DMA
    return pl.pallas_call(
        functools.partial(kernel, sizes),
        out_shape=jax.ShapeDtypeStruct((S, Q, D), BF16),
        in_specs=[hbm, vmem, hbm, hbm] + [vmem] * 10 + [hbm],
        out_specs=vmem,
        scratch_shapes=[
            pltpu.VMEM((tp, S, Q, D), BF16),
            pltpu.VMEM((D, W), BF16),
            pltpu.VMEM((D, W), BF16),
            pltpu.VMEM((tp, W, D), BF16),
            pltpu.VMEM((R, D), BF16),
            pltpu.VMEM((R, W), BF16),
            pltpu.VMEM((R, W), BF16),
            pltpu.VMEM((R, W), F32),
            pltpu.VMEM((tiles, mw, cw), BF16),
            pltpu.VMEM((tiles, mw, cw), BF16),
            pltpu.VMEM((tiles, cw, mw), BF16),
            pltpu.VMEM((tiles, cw, mw), BF16),
            pltpu.VMEM((tiles, Q, mw), F32),
            pltpu.VMEM((tiles, Q, mw), F32),
            pltpu.VMEM((tiles, Q, mw), F32),
            pltpu.VMEM((tiles, Q, mw), F32),
            pltpu.VMEM((tiles, R, mw), F32),
            pltpu.VMEM((tiles, R, mw), F32),
            pltpu.VMEM((tiles, tp * S, mw), F32),
            pltpu.VMEM((tiles, tp * S, mw), F32),
            pltpu.VMEM((8, G), F32),
            pltpu.VMEM((n, 8, G), F32),
            pltpu.VMEM((tiles, 2 * S, mw), BF16),
            pltpu.VMEM((n, tiles, 2 * S, mw), BF16),
            pltpu.VMEM((tp, S * Q, W), BF16),
            pltpu.VMEM((S * Q, W), BF16),
            dma((4,)),
            dma((3,)),
            dma((3,)),
            dma((n,)),
            dma((n,)),
            dma((n,)),
            dma((n,)),
        ],
        compiler_params=pltpu.CompilerParams(
            collective_id=0, has_side_effects=True, vmem_limit_bytes=60 * 1024 * 1024
        ),
    )(
        layer_input,
        norm_gain.reshape(1, D),
        in_weight,
        gate_weight,
        rate_real,
        rate_imag,
        log_step.reshape(1, G),
        input_real.reshape(G * N, C),
        input_imag.reshape(G * N, C),
        output_real.reshape(G * C, N),
        output_imag.reshape(G * C, N),
        skip_weight.reshape(1, W),
        decay_offset,
        channel_gain.reshape(tp, 1, W),
        out_weight,
    )


def solution(mesh):
    placed = (
        P("grp", ("sp", "tp"), None),
        P(),
        P(None, "tp"),
        P(None, "tp"),
        P("tp", None),
        P("tp", None),
        P("tp"),
        P("tp", None, None),
        P("tp", None, None),
        P("tp", None, None),
        P("tp", None, None),
        P("tp"),
        P("grp", "sp", "tp"),
        P(),
        P("tp", None),
    )
    body = functools.partial(shards, mesh.shape["sp"], mesh.shape["tp"])
    return jax.shard_map(
        body, mesh=mesh, in_specs=placed, out_specs=P("grp", ("sp", "tp"), None), check_vma=False
    )
```

```python
import functools

import jax
import jax.numpy as jnp
from jax import lax
from jax.experimental import pallas as pl
from jax.experimental.pallas import tpu as pltpu
from jax.sharding import PartitionSpec as P

epsilon = 1e-06
HIGHEST = lax.Precision.HIGHEST
MESH = pl.DeviceIdType.MESH
F32 = jnp.float32
BF16 = jnp.bfloat16


def iota(shape, dim):
    return lax.broadcasted_iota(jnp.int32, shape, dim)


def cmul(a, b):
    return (a[0] * b[0] - a[1] * b[1], a[0] * b[1] + a[1] * b[0])


def cpow(a, k):
    result = None
    while k:
        if k & 1:
            result = a if result is None else cmul(result, a)
        k >>= 1
        if k:
            a = cmul(a, a)
    return result


def dot(a, b, precision=None):
    return jnp.dot(a, b, preferred_element_type=F32, precision=precision)


def dot_nt(a, b, precision=None):
    return lax.dot_general(a, b, (((1,), (1,)), ((), ())), preferred_element_type=F32, precision=precision)


def kernel(
    sizes,
    x_hbm, ng_hbm, inw_hbm, gw_hbm, rr_hbm, ri_hbm, ls_hbm, bre_hbm, bim_hbm, cre_hbm, cim_hbm,
    skip_hbm, dec_hbm, cg_hbm, outw_hbm,
    out,
    ng, rr, ri, ls, bre, bim, cre, cim, skip, dec, cg,
    xf, w_in, w_g, w_o, nrm, u_ref, gate_ref, rel_ref,
    bd_re, bd_im, cd_re, cd_im, ti_re, ti_im, to_re, to_im,
    p_re, p_im, xc_re, xc_im, tot, tot_all, st, st_all, act, act_in,
    load_sem, small_sem, tp_send, tp_recv, tot_send, tot_recv, st_send, st_recv,
):
    n, tp, S, Q, D, G, N, C, tile_g, out_cols = sizes
    W = G * C
    tiles = G // tile_g
    cw, mw = tile_g * C, tile_g * N
    SQ = S * Q
    mid = Q // 2 - 1
    sp_me = lax.axis_index("sp")
    me = lax.axis_index("tp")
    peer = 1 - me

    barrier = pltpu.get_barrier_semaphore()
    pl.semaphore_signal(barrier, inc=1, device_id={"tp": peer}, device_id_type=MESH)

    def greet(i, carry):
        other = lax.rem(sp_me + 1 + i, n)
        pl.semaphore_signal(barrier, inc=1, device_id={"sp": other}, device_id_type=MESH)
        return carry

    lax.fori_loop(0, n - 1, greet, 0)

    load_x = pltpu.make_async_copy(x_hbm, xf.at[me], load_sem.at[0])
    load_in = pltpu.make_async_copy(inw_hbm, w_in, load_sem.at[1])
    load_g = pltpu.make_async_copy(gw_hbm, w_g, load_sem.at[2])
    load_o = pltpu.make_async_copy(outw_hbm, w_o.at[me], load_sem.at[3])
    small = [
        pltpu.make_async_copy(src, dst, small_sem.at[i])
        for i, (src, dst) in enumerate((
            (dec_hbm, dec), (ls_hbm, ls), (rr_hbm, rr), (ri_hbm, ri), (bre_hbm, bre), (bim_hbm, bim),
            (cre_hbm, cre), (cim_hbm, cim), (ng_hbm, ng), (skip_hbm, skip), (cg_hbm, cg),
        ))
    ]
    load_x.start()
    for copy in small:
        copy.start()
    load_in.start()
    load_g.start()
    load_o.start()

    small[0].wait()
    tri = (iota((Q, Q), 0) >= iota((Q, Q), 1)).astype(F32)
    to_chan = (iota((G, W), 1) // C == iota((G, W), 0)).astype(F32)
    mids, lasts, totals = [], [], []
    tot[...] = jnp.zeros_like(tot)
    for s in range(S):
        total = None
        for c in range(tp):
            cum = dot_nt(tri, dec[s, :, c * Q:(c + 1) * Q], HIGHEST)
            at_mid = cum[mid:mid + 1, :]
            at_end = cum[Q - 1:Q, :]
            mids.append(at_mid)
            lasts.append(at_end - at_mid)
            total = at_end if total is None else total + at_end
            rows = (c * S + s) * Q
            rel_ref[rows:rows + Q, :] = dot(cum - at_mid, to_chan, HIGHEST)
        totals.append(total)
        tot[s:s + 1, :] = total

    pl.semaphore_wait(barrier, n)

    load_x.wait()
    load_o.wait()
    send_x = pltpu.make_async_remote_copy(
        xf.at[me], xf.at[me], tp_send.at[0], tp_recv.at[0], device_id={"tp": peer}, device_id_type=MESH
    )
    send_o = pltpu.make_async_remote_copy(
        w_o.at[me], w_o.at[me], tp_send.at[1], tp_recv.at[1], device_id={"tp": peer}, device_id_type=MESH
    )
    send_x.start()
    send_o.start()

    def tot_copy(target):
        return pltpu.make_async_remote_copy(
            tot, tot_all.at[sp_me], tot_send.at[target], tot_recv.at[sp_me],
            device_id={"sp": target}, device_id_type=MESH,
        )

    def st_copy(target):
        return pltpu.make_async_remote_copy(
            st, st_all.at[sp_me], st_send.at[target], st_recv.at[sp_me],
            device_id={"sp": target}, device_id_type=MESH,
        )

    def to_later(act_on):
        def body(i, carry):
            act_on(n - 1 - i)
            return carry

        lax.fori_loop(0, n - 1 - sp_me, body, 0)

    to_later(lambda target: tot_copy(target).start())

    for copy in small[1:]:
        copy.wait()
    ls_row = jnp.broadcast_to(ls[...], (G, G))
    step = jnp.exp(jnp.sum(jnp.where(iota((G, G), 0) == iota((G, G), 1), ls_row, 0.0), axis=1, keepdims=True))
    rate_re, rate_im = rr[...], ri[...]
    real_step = rate_re * step
    angle_step = rate_im * step
    cosa, sina = jnp.cos(angle_step), jnp.sin(angle_step)
    half = jnp.sin(0.5 * angle_step)
    grown = jnp.exp(real_step)
    shrunk = jnp.exp(-real_step)
    series = jnp.ones_like(real_step)
    for k in range(11, 1, -1):
        series = 1.0 + real_step * (1.0 / k) * series
    minus_one = jnp.where(jnp.abs(real_step) < 0.5, real_step * series, grown - 1.0)
    top_re = minus_one * cosa - 2.0 * half * half
    top_im = grown * sina
    inverse = 1.0 / (rate_re * rate_re + rate_im * rate_im)
    coef_re = (top_re * rate_re + top_im * rate_im) * inverse
    coef_im = (top_im * rate_re - top_re * rate_im) * inverse
    spread = (iota((N, mw), 1) % N == iota((N, mw), 0)).astype(F32)
    to_mode = (iota((tile_g, mw), 1) // N == iota((tile_g, mw), 0)).astype(F32)

    def rows_of(item, q):
        wide = dot(item[q * tile_g:(q + 1) * tile_g, :], spread, HIGHEST)
        return jnp.sum(wide * to_mode, axis=0, keepdims=True)

    up_half, up_end, up_all = [], [], []
    k8 = iota((8, mw), 0)
    cmask = iota((cw, mw), 0) // C == iota((cw, mw), 1) // N
    ctile = spread.astype(BF16)

    def table(a, base, t_re, t_im, q):
        a2 = cmul(a, a)
        a4 = cmul(a2, a2)
        a8 = cmul(a4, a4)
        block = tuple(jnp.broadcast_to(b, (8, mw)) for b in base)
        for bit, power in ((1, a), (2, a2), (4, a4)):
            on = (k8 & bit) != 0
            block = cmul(block, (jnp.where(on, power[0], 1.0), jnp.where(on, power[1], 0.0)))
        for j in range(Q // 8):
            t_re[q, j * 8:j * 8 + 8, :] = block[0]
            t_im[q, j * 8:j * 8 + 8, :] = block[1]
            block = cmul(block, a8)

    for q in range(tiles):
        a = (rows_of(grown * cosa, q), rows_of(grown * sina, q))
        inv = (rows_of(shrunk * cosa, q), rows_of(-shrunk * sina, q))
        coef = (rows_of(coef_re, q), rows_of(coef_im, q))
        table(inv, cmul(coef, cpow(a, mid)), ti_re, ti_im, q)
        table(a, cpow(inv, mid), to_re, to_im, q)
        up_half.append(cpow(a, mid + 1))
        up_end.append(cpow(a, Q - 1 - mid))
        up_all.append(cpow(a, Q * tp))
        for src, dst in ((bre, bd_re), (bim, bd_im), (cre, cd_re), (cim, cd_im)):
            dst[q] = jnp.where(cmask, dot(src[q * cw:(q + 1) * cw, :], ctile), 0.0).astype(BF16)

    row_tile = min(32, Q)

    def project(slot):
        first = slot * SQ

        def normalize(i, carry):
            s = i // (Q // row_tile)
            r = pl.multiple_of((i % (Q // row_tile)) * row_tile, row_tile)
            x = xf[slot, s, pl.ds(r, row_tile), :].astype(F32)
            scale = lax.rsqrt(jnp.mean(x * x, axis=-1, keepdims=True) + epsilon)
            rows = pl.ds(pl.multiple_of(first + i * row_tile, row_tile), row_tile)
            nrm[rows, :] = (x * scale * ng[...]).astype(BF16)
            return carry

        lax.fori_loop(0, SQ // row_tile, normalize, 0)
        rows = pl.ds(pl.multiple_of(first, SQ), SQ)
        u_ref[rows, :] = dot(nrm[rows, :], w_in[...]).astype(BF16)

    load_in.wait()
    project(me)
    send_x.wait_recv()
    project(peer)

    R = tp * SQ
    ri_, ci_ = iota((R, R), 0), iota((R, R), 1)
    chunk_tri = ((ri_ >= ci_) & (ri_ // Q == ci_ // Q)).astype(BF16)

    for q in range(tiles):
        cols = slice(q * cw, (q + 1) * cw)
        uq = (u_ref[:, cols].astype(F32) * jnp.exp(-rel_ref[:, cols])).astype(BF16)
        d_re = dot(uq, bd_re[q]).reshape(tp * S, Q, mw)
        d_im = dot(uq, bd_im[q]).reshape(tp * S, Q, mw)
        t = (ti_re[q][None], ti_im[q][None])
        z_re, z_im = cmul(t, (d_re, d_im))
        p_re[q] = dot(chunk_tri, z_re.reshape(R, mw).astype(BF16))
        p_im[q] = dot(chunk_tri, z_im.reshape(R, mw).astype(BF16))

    def widen(row, q):
        return jnp.exp(dot(jnp.broadcast_to(row[:, q * tile_g:(q + 1) * tile_g], (8, tile_g)), to_mode, HIGHEST)[0:1])

    enter_f, leave_f = {}, {}
    for q in range(tiles):
        for s in range(S):
            x = None
            for c in range(tp):
                b = c * S + s
                e_mid = widen(mids[s * tp + c], q)
                e_end = widen(lasts[s * tp + c], q)
                enter_f[q, s, c] = (up_half[q][0] * e_mid, up_half[q][1] * e_mid)
                leave_f[q, s, c] = (up_end[q][0] * e_end, up_end[q][1] * e_end)
                last = b * Q + Q - 1
                end = (p_re[q, last:last + 1, :], p_im[q, last:last + 1, :])
                if x is not None:
                    add = cmul(enter_f[q, s, c], x)
                    end = (end[0] + add[0], end[1] + add[1])
                x = cmul(leave_f[q, s, c], end)
            st[q, s:s + 1, :] = x[0].astype(BF16)
            st[q, S + s:S + s + 1, :] = x[1].astype(BF16)

    to_later(lambda target: st_copy(target).start())

    load_g.wait()
    gate_ref[...] = dot(nrm[...], w_g[...]).astype(BF16)

    def enter(j, x):
        pltpu.make_async_remote_copy(
            tot, tot_all.at[j], tot_send.at[j], tot_recv.at[j], device_id={"tp": peer}, device_id_type=MESH
        ).wait_recv()
        pltpu.make_async_remote_copy(
            st, st_all.at[j], st_send.at[j], st_recv.at[j], device_id={"tp": peer}, device_id_type=MESH
        ).wait_recv()
        logs = tot_all[j]
        new = []
        for q in range(tiles):
            decay = jnp.exp(dot(logs[:, q * tile_g:(q + 1) * tile_g], to_mode, HIGHEST))[0:S]
            got = st_all[j, q].astype(F32)
            re, im = cmul((up_all[q][0] * decay, up_all[q][1] * decay), x[q])
            new.append((re + got[0:S], im + got[S:2 * S]))
        return tuple(new)

    zero = jnp.zeros((S, mw), F32)
    entering = lax.fori_loop(0, sp_me, enter, tuple((zero, zero) for _ in range(tiles)))

    for q in range(tiles):
        for s in range(S):
            x = (entering[q][0][s:s + 1], entering[q][1][s:s + 1])
            for c in range(tp):
                b = c * S + s
                add = cmul(enter_f[q, s, c], x)
                xc_re[q, b:b + 1, :] = add[0]
                xc_im[q, b:b + 1, :] = add[1]
                if c < tp - 1:
                    last = b * Q + Q - 1
                    x = cmul(
                        leave_f[q, s, c],
                        (p_re[q, last:last + 1, :] + add[0], p_im[q, last:last + 1, :] + add[1]),
                    )

    def read_out(slot, dst):
        first = pl.multiple_of(slot * SQ, SQ)
        rows = pl.ds(first, SQ)
        for q in range(tiles):
            cols = slice(q * cw, (q + 1) * cw)
            acc_re, acc_im = [], []
            for s in range(S):
                block = pl.ds(pl.multiple_of(first + s * Q, Q), Q)
                one = pl.ds(slot * S + s, 1)
                v = (p_re[q, block, :] + xc_re[q, one, :], p_im[q, block, :] + xc_im[q, one, :])
                w = cmul((to_re[q], to_im[q]), v)
                acc_re.append(w[0].astype(BF16))
                acc_im.append(w[1].astype(BF16))
            w_re = jnp.concatenate(acc_re, axis=0)
            w_im = jnp.concatenate(acc_im, axis=0)
            y = dot_nt(w_re, cd_re[q]) - dot_nt(w_im, cd_im[q])
            mixed = y * jnp.exp(rel_ref[rows, cols]) + skip[:, cols] * u_ref[rows, cols].astype(F32)
            gate = jax.nn.sigmoid(gate_ref[rows, cols].astype(F32))
            gelu = 0.5 * mixed * (1.0 + lax.erf(mixed * 0.7071067811865476))
            dst[:, cols] = (gelu * gate).astype(BF16)

    read_out(peer, act.at[peer])
    send_a = pltpu.make_async_remote_copy(
        act.at[peer], act_in, tp_send.at[2], tp_recv.at[2], device_id={"tp": peer}, device_id_type=MESH
    )
    send_a.start()
    read_out(me, act.at[me])
    own = act[me].astype(F32)
    own_sq = jnp.sum(own * own, axis=-1, keepdims=True)
    own_g = (own * cg[me]).astype(BF16)
    send_o.wait_recv()
    send_a.wait_recv()
    got = act_in[...].astype(F32)
    got_sq = jnp.sum(got * got, axis=-1, keepdims=True)
    got_g = (got * cg[peer]).astype(BF16)
    scale = lax.rsqrt((own_sq + got_sq) * (1.0 / (tp * W)) + epsilon)
    for k in range(D // out_cols):
        cols = slice(k * out_cols, (k + 1) * out_cols)
        y = dot(own_g, w_o[me, :, cols]) + dot(got_g, w_o[peer, :, cols])
        out[:, :, cols] = (y * scale).astype(BF16).reshape(S, Q, out_cols)

    send_x.wait_send()
    send_o.wait_send()
    send_a.wait_send()
    to_later(lambda target: tot_copy(target).wait_send())
    to_later(lambda target: st_copy(target).wait_send())


def shards(
    n, tp, layer_input, norm_gain, in_weight, gate_weight, rate_real, rate_imag, log_step, input_real,
    input_imag, output_real, output_imag, skip_weight, decay_offset, channel_gain, out_weight,
):
    S, Q, D = layer_input.shape
    G, N = rate_real.shape
    C = input_real.shape[2]
    W = G * C
    tile_g = min(G, max(1, 128 // C))
    tiles = G // tile_g
    cw, mw = tile_g * C, tile_g * N
    R = tp * S * Q
    assert tp == 2 and Q <= 64 and Q % 8 == 0
    sizes = (n, tp, S, Q, D, G, N, C, tile_g, min(512, D))
    vmem = pl.BlockSpec(memory_space=pltpu.VMEM)
    hbm = pl.BlockSpec(memory_space=pltpu.HBM)
    dma = pltpu.SemaphoreType.DMA
    return pl.pallas_call(
        functools.partial(kernel, sizes),
        out_shape=jax.ShapeDtypeStruct((S, Q, D), BF16),
        in_specs=[hbm] * 15,
        out_specs=vmem,
        scratch_shapes=[
            pltpu.VMEM((1, D), F32),
            pltpu.VMEM((G, N), F32),
            pltpu.VMEM((G, N), F32),
            pltpu.VMEM((1, G), F32),
            pltpu.VMEM((W, N), BF16),
            pltpu.VMEM((W, N), BF16),
            pltpu.VMEM((W, N), BF16),
            pltpu.VMEM((W, N), BF16),
            pltpu.VMEM((1, W), F32),
            pltpu.VMEM((S, G, tp * Q), F32),
            pltpu.VMEM((tp, 1, W), F32),
            pltpu.VMEM((tp, S, Q, D), BF16),
            pltpu.VMEM((D, W), BF16),
            pltpu.VMEM((D, W), BF16),
            pltpu.VMEM((tp, W, D), BF16),
            pltpu.VMEM((R, D), BF16),
            pltpu.VMEM((R, W), BF16),
            pltpu.VMEM((R, W), BF16),
            pltpu.VMEM((R, W), F32),
            pltpu.VMEM((tiles, cw, mw), BF16),
            pltpu.VMEM((tiles, cw, mw), BF16),
            pltpu.VMEM((tiles, cw, mw), BF16),
            pltpu.VMEM((tiles, cw, mw), BF16),
            pltpu.VMEM((tiles, Q, mw), F32),
            pltpu.VMEM((tiles, Q, mw), F32),
            pltpu.VMEM((tiles, Q, mw), F32),
            pltpu.VMEM((tiles, Q, mw), F32),
            pltpu.VMEM((tiles, R, mw), F32),
            pltpu.VMEM((tiles, R, mw), F32),
            pltpu.VMEM((tiles, tp * S, mw), F32),
            pltpu.VMEM((tiles, tp * S, mw), F32),
            pltpu.VMEM((8, G), F32),
            pltpu.VMEM((n, 8, G), F32),
            pltpu.VMEM((tiles, 2 * S, mw), BF16),
            pltpu.VMEM((n, tiles, 2 * S, mw), BF16),
            pltpu.VMEM((tp, S * Q, W), BF16),
            pltpu.VMEM((S * Q, W), BF16),
            dma((4,)),
            dma((11,)),
            dma((3,)),
            dma((3,)),
            dma((n,)),
            dma((n,)),
            dma((n,)),
            dma((n,)),
        ],
        compiler_params=pltpu.CompilerParams(
            collective_id=0, has_side_effects=True, vmem_limit_bytes=60 * 1024 * 1024
        ),
    )(
        layer_input,
        norm_gain.reshape(1, D),
        in_weight,
        gate_weight,
        rate_real,
        rate_imag,
        log_step.reshape(1, G),
        jnp.swapaxes(input_real, 1, 2).reshape(G * C, N),
        jnp.swapaxes(input_imag, 1, 2).reshape(G * C, N),
        output_real.reshape(G * C, N),
        output_imag.reshape(G * C, N),
        skip_weight.reshape(1, W),
        jnp.swapaxes(decay_offset, 1, 2),
        channel_gain.reshape(tp, 1, W),
        out_weight,
    )


def solution(mesh):
    placed = (
        P("grp", ("sp", "tp"), None),
        P(),
        P(None, "tp"),
        P(None, "tp"),
        P("tp", None),
        P("tp", None),
        P("tp"),
        P("tp", None, None),
        P("tp", None, None),
        P("tp", None, None),
        P("tp", None, None),
        P("tp"),
        P("grp", "sp", "tp"),
        P(),
        P("tp", None),
    )
    body = functools.partial(shards, mesh.shape["sp"], mesh.shape["tp"])
    return jax.shard_map(
        body, mesh=mesh, in_specs=placed, out_specs=P("grp", ("sp", "tp"), None), check_vma=False
    )
```

```python
import functools

import jax
import jax.numpy as jnp
from jax import lax
from jax.experimental import pallas as pl
from jax.experimental.pallas import tpu as pltpu
from jax.sharding import PartitionSpec as P

epsilon = 1e-06
HIGHEST = lax.Precision.HIGHEST
MESH = pl.DeviceIdType.MESH
F32 = jnp.float32
BF16 = jnp.bfloat16


def iota(shape, dim):
    return lax.broadcasted_iota(jnp.int32, shape, dim)


def cmul(a, b):
    return (a[0] * b[0] - a[1] * b[1], a[0] * b[1] + a[1] * b[0])


def cpow(a, k):
    result = None
    while k:
        if k & 1:
            result = a if result is None else cmul(result, a)
        k >>= 1
        if k:
            a = cmul(a, a)
    return result


def dot(a, b, precision=None):
    return jnp.dot(a, b, preferred_element_type=F32, precision=precision)


def dot_nt(a, b, precision=None):
    return lax.dot_general(a, b, (((1,), (1,)), ((), ())), preferred_element_type=F32, precision=precision)


def kernel(
    sizes,
    x_hbm, ng_hbm, inw_hbm, gw_hbm, rr_hbm, ri_hbm, ls_hbm, bre_hbm, bim_hbm, cre_hbm, cim_hbm,
    skip_hbm, dec_hbm, cg_hbm, outw_hbm,
    out,
    ng, rr, ri, ls, bre, bim, cre, cim, skip, dec, cg,
    xf, w_in, w_g, w_o, nrm, u_ref, gate_ref, rel_ref,
    bd_re, bd_im, cd_re, cd_im, ti_re, ti_im, to_re, to_im,
    p_re, p_im, xc_re, xc_im, tot, tot_all, st, st_all, act, act_in, chunk_decay, across_re, across_im, acc,
    load_sem, small_sem, tp_send, tp_recv, tot_send, tot_recv, st_send, st_recv,
):
    n, tp, S, Q, D, G, N, C, tile_g, out_cols = sizes
    W = G * C
    tiles = G // tile_g
    cw, mw = tile_g * C, tile_g * N
    SQ = S * Q
    mid = Q // 2 - 1
    sp_me = lax.axis_index("sp")
    me = lax.axis_index("tp")
    peer = 1 - me

    barrier = pltpu.get_barrier_semaphore()
    pl.semaphore_signal(barrier, inc=1, device_id={"tp": peer}, device_id_type=MESH)

    def greet(i, carry):
        other = lax.rem(sp_me + 1 + i, n)
        pl.semaphore_signal(barrier, inc=1, device_id={"sp": other}, device_id_type=MESH)
        return carry

    lax.fori_loop(0, n - 1, greet, 0)

    load_x = pltpu.make_async_copy(x_hbm, xf.at[me], load_sem.at[0])
    load_in = pltpu.make_async_copy(inw_hbm, w_in, load_sem.at[1])
    load_g = pltpu.make_async_copy(gw_hbm, w_g, load_sem.at[2])
    load_o = pltpu.make_async_copy(outw_hbm, w_o.at[me], load_sem.at[3])
    small = [
        pltpu.make_async_copy(src, dst, small_sem.at[i])
        for i, (src, dst) in enumerate((
            (dec_hbm, dec), (ls_hbm, ls), (rr_hbm, rr), (ri_hbm, ri), (bre_hbm, bre), (bim_hbm, bim),
            (cre_hbm, cre), (cim_hbm, cim), (ng_hbm, ng), (skip_hbm, skip), (cg_hbm, cg),
        ))
    ]
    load_x.start()
    for copy in small:
        copy.start()
    load_in.start()
    load_g.start()
    load_o.start()

    small[0].wait()
    tri = (iota((Q, Q), 0) >= iota((Q, Q), 1)).astype(F32)
    to_chan = (iota((G, W), 1) // C == iota((G, W), 0)).astype(F32)
    mids, lasts, totals = [], [], []
    tot[...] = jnp.zeros_like(tot)
    for s in range(S):
        total = None
        for c in range(tp):
            cum = dot_nt(tri, dec[s, :, c * Q:(c + 1) * Q], HIGHEST)
            at_mid = cum[mid:mid + 1, :]
            at_end = cum[Q - 1:Q, :]
            mids.append(at_mid)
            lasts.append(at_end - at_mid)
            total = at_end if total is None else total + at_end
            rows = (c * S + s) * Q
            rel_ref[rows:rows + Q, :] = dot(cum - at_mid, to_chan, HIGHEST)
        tot[s:s + 1, :] = total

    to_mode = (iota((tile_g, mw), 1) // N == iota((tile_g, mw), 0)).astype(F32)
    logs = jnp.concatenate(mids + lasts, axis=0)

    def widen(rows, q):
        return jnp.exp(dot(rows[:, q * tile_g:(q + 1) * tile_g], to_mode, HIGHEST))

    for q in range(tiles):
        chunk_decay[q] = widen(logs, q)

    send_x = pltpu.make_async_remote_copy(
        xf.at[me], xf.at[me], tp_send.at[0], tp_recv.at[0], device_id={"tp": peer}, device_id_type=MESH
    )
    send_o = pltpu.make_async_remote_copy(
        w_o.at[me], w_o.at[me], tp_send.at[1], tp_recv.at[1], device_id={"tp": peer}, device_id_type=MESH
    )
    def tot_copy(target):
        return pltpu.make_async_remote_copy(
            tot, tot_all.at[sp_me], tot_send.at[target], tot_recv.at[sp_me],
            device_id={"sp": target}, device_id_type=MESH,
        )

    def st_copy(target):
        return pltpu.make_async_remote_copy(
            st, st_all.at[sp_me], st_send.at[target], st_recv.at[sp_me],
            device_id={"sp": target}, device_id_type=MESH,
        )

    def to_later(act_on):
        def body(i, carry):
            act_on(n - 1 - i)
            return carry

        lax.fori_loop(0, n - 1 - sp_me, body, 0)

    for copy in small[1:]:
        copy.wait()
    ls_row = jnp.broadcast_to(ls[...], (G, G))
    step = jnp.exp(jnp.sum(jnp.where(iota((G, G), 0) == iota((G, G), 1), ls_row, 0.0), axis=1, keepdims=True))
    rate_re, rate_im = rr[...], ri[...]
    real_step = rate_re * step
    angle_step = rate_im * step
    cosa, sina = jnp.cos(angle_step), jnp.sin(angle_step)
    half = jnp.sin(0.5 * angle_step)
    grown = jnp.exp(real_step)
    shrunk = jnp.exp(-real_step)
    series = jnp.ones_like(real_step)
    for k in range(11, 1, -1):
        series = 1.0 + real_step * (1.0 / k) * series
    minus_one = jnp.where(jnp.abs(real_step) < 0.5, real_step * series, grown - 1.0)
    top_re = minus_one * cosa - 2.0 * half * half
    top_im = grown * sina
    inverse = 1.0 / (rate_re * rate_re + rate_im * rate_im)
    coef_re = (top_re * rate_re + top_im * rate_im) * inverse
    coef_im = (top_im * rate_re - top_re * rate_im) * inverse
    spread = (iota((N, mw), 1) % N == iota((N, mw), 0)).astype(F32)
    def rows_of(item, q):
        wide = dot(item[q * tile_g:(q + 1) * tile_g, :], spread, HIGHEST)
        return jnp.sum(wide * to_mode, axis=0, keepdims=True)

    up_half, up_end, up_all = [], [], []
    k8 = iota((8, mw), 0)
    cmask = iota((cw, mw), 0) // C == iota((cw, mw), 1) // N
    ctile = spread.astype(BF16)

    def table(a, base, t_re, t_im, q):
        a2 = cmul(a, a)
        a4 = cmul(a2, a2)
        a8 = cmul(a4, a4)
        block = tuple(jnp.broadcast_to(b, (8, mw)) for b in base)
        for bit, power in ((1, a), (2, a2), (4, a4)):
            on = (k8 & bit) != 0
            block = cmul(block, (jnp.where(on, power[0], 1.0), jnp.where(on, power[1], 0.0)))
        for j in range(Q // 8):
            t_re[q, j * 8:j * 8 + 8, :] = block[0]
            t_im[q, j * 8:j * 8 + 8, :] = block[1]
            block = cmul(block, a8)

    for q in range(tiles):
        if q == tiles // 2:
            pl.semaphore_wait(barrier, n)
            load_x.wait()
            send_x.start()
            to_later(lambda target: tot_copy(target).start())
        a = (rows_of(grown * cosa, q), rows_of(grown * sina, q))
        inv = (rows_of(shrunk * cosa, q), rows_of(-shrunk * sina, q))
        coef = (rows_of(coef_re, q), rows_of(coef_im, q))
        table(inv, cmul(coef, cpow(a, mid)), ti_re, ti_im, q)
        table(a, cpow(inv, mid), to_re, to_im, q)
        up_half.append(cpow(a, mid + 1))
        up_end.append(cpow(a, Q - 1 - mid))
        up_all.append(cpow(a, Q * tp))
        for src, dst in ((bre, bd_re), (bim, bd_im), (cre, cd_re), (cim, cd_im)):
            dst[q] = jnp.where(cmask, dot(src[q * cw:(q + 1) * cw, :], ctile), 0.0).astype(BF16)

    row_tile = min(32, Q)

    def project(slot):
        first = slot * SQ

        def normalize(i, carry):
            s = i // (Q // row_tile)
            r = pl.multiple_of((i % (Q // row_tile)) * row_tile, row_tile)
            x = xf[slot, s, pl.ds(r, row_tile), :].astype(F32)
            scale = lax.rsqrt(jnp.mean(x * x, axis=-1, keepdims=True) + epsilon)
            rows = pl.ds(pl.multiple_of(first + i * row_tile, row_tile), row_tile)
            nrm[rows, :] = (x * scale * ng[...]).astype(BF16)
            return carry

        lax.fori_loop(0, SQ // row_tile, normalize, 0)
        rows = pl.ds(pl.multiple_of(first, SQ), SQ)
        u_ref[rows, :] = dot(nrm[rows, :], w_in[...]).astype(BF16)

    load_o.wait()
    send_o.start()
    load_in.wait()
    project(me)
    send_x.wait_recv()
    project(peer)

    R = tp * SQ
    ri_, ci_ = iota((R, R), 0), iota((R, R), 1)
    chunk_tri = ((ri_ >= ci_) & (ri_ // Q == ci_ // Q)).astype(BF16)

    for q in range(tiles):
        cols = slice(q * cw, (q + 1) * cw)
        uq = (u_ref[:, cols].astype(F32) * jnp.exp(-rel_ref[:, cols])).astype(BF16)
        d_re = dot(uq, bd_re[q]).reshape(tp * S, Q, mw)
        d_im = dot(uq, bd_im[q]).reshape(tp * S, Q, mw)
        t = (ti_re[q][None], ti_im[q][None])
        z_re, z_im = cmul(t, (d_re, d_im))
        p_re[q] = dot(chunk_tri, z_re.reshape(R, mw).astype(BF16))
        p_im[q] = dot(chunk_tri, z_im.reshape(R, mw).astype(BF16))

    enter_f, leave_f = {}, {}
    for q in range(tiles):
        for s in range(S):
            x = None
            for c in range(tp):
                b = c * S + s
                k = s * tp + c
                e_mid = chunk_decay[q, k:k + 1, :]
                e_end = chunk_decay[q, S * tp + k:S * tp + k + 1, :]
                enter_f[q, s, c] = (up_half[q][0] * e_mid, up_half[q][1] * e_mid)
                leave_f[q, s, c] = (up_end[q][0] * e_end, up_end[q][1] * e_end)
                last = b * Q + Q - 1
                end = (p_re[q, last:last + 1, :], p_im[q, last:last + 1, :])
                if x is not None:
                    add = cmul(enter_f[q, s, c], x)
                    end = (end[0] + add[0], end[1] + add[1])
                x = cmul(leave_f[q, s, c], end)
            st[q, s:s + 1, :] = x[0].astype(BF16)
            st[q, S + s:S + s + 1, :] = x[1].astype(BF16)

    to_later(lambda target: st_copy(target).start())

    load_g.wait()
    gate_ref[...] = dot(nrm[...], w_g[...]).astype(BF16)

    def tot_here(j, carry):
        pltpu.make_async_remote_copy(
            tot, tot_all.at[j], tot_send.at[j], tot_recv.at[j], device_id={"tp": peer}, device_id_type=MESH
        ).wait_recv()
        return carry

    lax.fori_loop(0, sp_me, tot_here, 0)
    all_logs = tot_all[...].reshape(n * 8, G)
    for q in range(tiles):
        decay = widen(all_logs, q)
        across_re[:, q] = (up_all[q][0] * decay).reshape(n, 8, mw)
        across_im[:, q] = (up_all[q][1] * decay).reshape(n, 8, mw)

    def enter(j, x):
        pltpu.make_async_remote_copy(
            st, st_all.at[j], st_send.at[j], st_recv.at[j], device_id={"tp": peer}, device_id_type=MESH
        ).wait_recv()
        new = []
        for q in range(tiles):
            got = st_all[j, q].astype(F32)
            re, im = cmul((across_re[j, q, 0:S], across_im[j, q, 0:S]), x[q])
            new.append((re + got[0:S], im + got[S:2 * S]))
        return tuple(new)

    zero = jnp.zeros((S, mw), F32)
    entering = lax.fori_loop(0, sp_me, enter, tuple((zero, zero) for _ in range(tiles)))

    for q in range(tiles):
        for s in range(S):
            x = (entering[q][0][s:s + 1], entering[q][1][s:s + 1])
            for c in range(tp):
                b = c * S + s
                add = cmul(enter_f[q, s, c], x)
                xc_re[q, b:b + 1, :] = add[0]
                xc_im[q, b:b + 1, :] = add[1]
                if c < tp - 1:
                    last = b * Q + Q - 1
                    x = cmul(
                        leave_f[q, s, c],
                        (p_re[q, last:last + 1, :] + add[0], p_im[q, last:last + 1, :] + add[1]),
                    )

    def read_out(slot, dst):
        first = pl.multiple_of(slot * SQ, SQ)
        rows = pl.ds(first, SQ)
        for q in range(tiles):
            cols = slice(q * cw, (q + 1) * cw)
            acc_re, acc_im = [], []
            for s in range(S):
                block = pl.ds(pl.multiple_of(first + s * Q, Q), Q)
                one = pl.ds(slot * S + s, 1)
                v = (p_re[q, block, :] + xc_re[q, one, :], p_im[q, block, :] + xc_im[q, one, :])
                w = cmul((to_re[q], to_im[q]), v)
                acc_re.append(w[0].astype(BF16))
                acc_im.append(w[1].astype(BF16))
            w_re = jnp.concatenate(acc_re, axis=0)
            w_im = jnp.concatenate(acc_im, axis=0)
            y = dot_nt(w_re, cd_re[q]) - dot_nt(w_im, cd_im[q])
            mixed = y * jnp.exp(rel_ref[rows, cols]) + skip[:, cols] * u_ref[rows, cols].astype(F32)
            gate = jax.nn.sigmoid(gate_ref[rows, cols].astype(F32))
            gelu = 0.5 * mixed * (1.0 + lax.erf(mixed * 0.7071067811865476))
            dst[:, cols] = (gelu * gate).astype(BF16)

    read_out(peer, act.at[peer])
    send_a = pltpu.make_async_remote_copy(
        act.at[peer], act_in, tp_send.at[2], tp_recv.at[2], device_id={"tp": peer}, device_id_type=MESH
    )
    send_a.start()
    read_out(me, act.at[me])
    own = act[me].astype(F32)
    own_sq = jnp.sum(own * own, axis=-1, keepdims=True)
    own_g = (own * cg[me]).astype(BF16)
    for k in range(D // out_cols):
        cols = slice(k * out_cols, (k + 1) * out_cols)
        acc[:, cols] = dot(own_g, w_o[me, :, cols])
    send_o.wait_recv()
    send_a.wait_recv()
    got = act_in[...].astype(F32)
    got_sq = jnp.sum(got * got, axis=-1, keepdims=True)
    got_g = (got * cg[peer]).astype(BF16)
    scale = lax.rsqrt((own_sq + got_sq) * (1.0 / (tp * W)) + epsilon)
    for k in range(D // out_cols):
        cols = slice(k * out_cols, (k + 1) * out_cols)
        y = acc[:, cols] + dot(got_g, w_o[peer, :, cols])
        out[:, :, cols] = (y * scale).astype(BF16).reshape(S, Q, out_cols)

    send_x.wait_send()
    send_o.wait_send()
    send_a.wait_send()
    to_later(lambda target: tot_copy(target).wait_send())
    to_later(lambda target: st_copy(target).wait_send())


def shards(
    n, tp, layer_input, norm_gain, in_weight, gate_weight, rate_real, rate_imag, log_step, input_real,
    input_imag, output_real, output_imag, skip_weight, decay_offset, channel_gain, out_weight,
):
    S, Q, D = layer_input.shape
    G, N = rate_real.shape
    C = input_real.shape[2]
    W = G * C
    tile_g = min(G, max(1, 128 // C))
    tiles = G // tile_g
    cw, mw = tile_g * C, tile_g * N
    R = tp * S * Q
    assert tp == 2 and Q <= 64 and Q % 8 == 0
    sizes = (n, tp, S, Q, D, G, N, C, tile_g, min(512, D))
    vmem = pl.BlockSpec(memory_space=pltpu.VMEM)
    hbm = pl.BlockSpec(memory_space=pltpu.HBM)
    dma = pltpu.SemaphoreType.DMA
    return pl.pallas_call(
        functools.partial(kernel, sizes),
        out_shape=jax.ShapeDtypeStruct((S, Q, D), BF16),
        in_specs=[hbm] * 15,
        out_specs=vmem,
        scratch_shapes=[
            pltpu.VMEM((1, D), F32),
            pltpu.VMEM((G, N), F32),
            pltpu.VMEM((G, N), F32),
            pltpu.VMEM((1, G), F32),
            pltpu.VMEM((W, N), BF16),
            pltpu.VMEM((W, N), BF16),
            pltpu.VMEM((W, N), BF16),
            pltpu.VMEM((W, N), BF16),
            pltpu.VMEM((1, W), F32),
            pltpu.VMEM((S, G, tp * Q), F32),
            pltpu.VMEM((tp, 1, W), F32),
            pltpu.VMEM((tp, S, Q, D), BF16),
            pltpu.VMEM((D, W), BF16),
            pltpu.VMEM((D, W), BF16),
            pltpu.VMEM((tp, W, D), BF16),
            pltpu.VMEM((R, D), BF16),
            pltpu.VMEM((R, W), BF16),
            pltpu.VMEM((R, W), BF16),
            pltpu.VMEM((R, W), F32),
            pltpu.VMEM((tiles, cw, mw), BF16),
            pltpu.VMEM((tiles, cw, mw), BF16),
            pltpu.VMEM((tiles, cw, mw), BF16),
            pltpu.VMEM((tiles, cw, mw), BF16),
            pltpu.VMEM((tiles, Q, mw), F32),
            pltpu.VMEM((tiles, Q, mw), F32),
            pltpu.VMEM((tiles, Q, mw), F32),
            pltpu.VMEM((tiles, Q, mw), F32),
            pltpu.VMEM((tiles, R, mw), F32),
            pltpu.VMEM((tiles, R, mw), F32),
            pltpu.VMEM((tiles, tp * S, mw), F32),
            pltpu.VMEM((tiles, tp * S, mw), F32),
            pltpu.VMEM((8, G), F32),
            pltpu.VMEM((n, 8, G), F32),
            pltpu.VMEM((tiles, 2 * S, mw), BF16),
            pltpu.VMEM((n, tiles, 2 * S, mw), BF16),
            pltpu.VMEM((tp, S * Q, W), BF16),
            pltpu.VMEM((S * Q, W), BF16),
            pltpu.VMEM((tiles, 2 * S * tp, mw), F32),
            pltpu.VMEM((n, tiles, 8, mw), F32),
            pltpu.VMEM((n, tiles, 8, mw), F32),
            pltpu.VMEM((S * Q, D), F32),
            dma((4,)),
            dma((11,)),
            dma((3,)),
            dma((3,)),
            dma((n,)),
            dma((n,)),
            dma((n,)),
            dma((n,)),
        ],
        compiler_params=pltpu.CompilerParams(
            collective_id=0, has_side_effects=True, vmem_limit_bytes=60 * 1024 * 1024
        ),
    )(
        layer_input,
        norm_gain.reshape(1, D),
        in_weight,
        gate_weight,
        rate_real,
        rate_imag,
        log_step.reshape(1, G),
        jnp.swapaxes(input_real, 1, 2).reshape(G * C, N),
        jnp.swapaxes(input_imag, 1, 2).reshape(G * C, N),
        output_real.reshape(G * C, N),
        output_imag.reshape(G * C, N),
        skip_weight.reshape(1, W),
        jnp.swapaxes(decay_offset, 1, 2),
        channel_gain.reshape(tp, 1, W),
        out_weight,
    )


def solution(mesh):
    placed = (
        P("grp", ("sp", "tp"), None),
        P(),
        P(None, "tp"),
        P(None, "tp"),
        P("tp", None),
        P("tp", None),
        P("tp"),
        P("tp", None, None),
        P("tp", None, None),
        P("tp", None, None),
        P("tp", None, None),
        P("tp"),
        P("grp", "sp", "tp"),
        P(),
        P("tp", None),
    )
    body = functools.partial(shards, mesh.shape["sp"], mesh.shape["tp"])
    return jax.shard_map(
        body, mesh=mesh, in_specs=placed, out_specs=P("grp", ("sp", "tp"), None), check_vma=False
    )
```
